32 devices in a mesh: sp: 8 (over z, x), tp: 4 (over y, core).
Axes of the slice: x: 2, y: 2, z: 4, core: 2. Of those that a mesh axis runs over, the one named last changes fastest.
Arguments:
- resid: bfloat16 [6144, 2048], P(('sp', 'tp')), may hold values from -6 to 6
- queries: bfloat16 [6144, 1024], P('sp', 'tp'), may hold values from -160 to 160
- keys: bfloat16 [6144, 1024], P('sp', 'tp'), may hold values from -6 to 6
- values: bfloat16 [6144, 1024], P('sp', 'tp'), may hold values from -6 to 6
- cum_gate: float32 [6144, 16], P('sp', 'tp'), may hold values from -694 to 0, as said below
- out_weight: bfloat16 [1024, 2048], P('tp'), may hold values from -0.375 to 0.375
- norm_gain: float32 [2048], replicated, may hold values from 0.1 to 1.9
- gate_weight: bfloat16 [2048, 5504], P('sp', 'tp'), may hold values from -0.125 to 0.125
- up_weight: bfloat16 [2048, 5504], P('sp', 'tp'), may hold values from -0.125 to 0.125
- down_weight: bfloat16 [5504, 2048], P('tp', 'sp'), may hold values from -0.078125 to 0.078125
Outputs:
- layer_out: bfloat16 [6144, 2048], P(('sp', 'tp'))
The draws below stay inside these ranges and needn't reach their ends.
Inputs may be any that keep to these rules, and one draw needn't show every extreme that they name: `cum_gate`: each column is non-increasing along positions and starts at or below zero.
All inputs are finite; a program needn't handle non-finite values.
Results may differ from the reference program's by a relative error of at most 0.01.
Values may be sent and summed in bfloat16 or wider, within the bound.
A program may use at most 256 MiB of HBM per device.

```python
import jax
import jax.numpy as jnp
from jax import lax

D = 2048
HEAD_COUNT = 16
HEAD_DIM = 64
FF = 5504
TOK_DEV = 768
TOKEN_COUNT = 6144
N_SP = 8
N_TP = 4


def paired_rows(key):
    key_query, key_key = jax.random.split(jax.random.fold_in(key, 11))
    width = HEAD_COUNT * HEAD_DIM
    queries = 2.5 * jnp.clip(jax.random.normal(key_query, (TOKEN_COUNT, width), jnp.float32), -5.0, 5.0)
    keys = jnp.clip(jax.random.normal(key_key, (TOKEN_COUNT, width), jnp.float32), -5.0, 5.0)
    return (queries, keys)


def draw_queries(key, part):
    return paired_rows(key)[0].astype(jnp.bfloat16)


def draw_keys(key, part):
    return paired_rows(key)[1].astype(jnp.bfloat16)


def draw_cum_gate(key, part):
    key_fast, key_block, key_rough, key_index_offset, key_length = jax.random.split(jax.random.fold_in(key, 23), 5)
    fast = jax.random.randint(key_fast, (HEAD_COUNT,), 0, 2).astype(jnp.float32)
    blocks = TOKEN_COUNT // TOK_DEV
    block_factor = jnp.exp(jax.random.uniform(key_block, (blocks, 1), jnp.float32, 0.0, jnp.log(3.0)))
    block_factor = jnp.repeat(block_factor, TOK_DEV, axis=0)
    rough = jax.random.uniform(key_rough, (TOKEN_COUNT, HEAD_COUNT), jnp.float32, 0.5, 1.5)
    base = fast * (1.0 / 40.0) + (1.0 - fast) * (0.6 / TOKEN_COUNT)
    stride_offset = -base[None, :] * block_factor * rough
    group_row_block = jax.random.randint(key_index_offset, (4,), 0, TOKEN_COUNT)
    group_row_count = jnp.log(jax.random.uniform(key_length, (4, HEAD_COUNT), jnp.float32, 0.5, 0.8))
    stride_offset = stride_offset.at[group_row_block].add(group_row_count)
    return jnp.cumsum(stride_offset, axis=0)


def block_scale(key, dims, shards, least, largest):
    def one(dim, parts):
        draws = jax.random.uniform(jax.random.fold_in(jax.random.fold_in(key, 6), dim), (parts,), jnp.float32, least / len(shards), largest / len(shards))
        return jnp.repeat(jnp.exp(draws), dims[dim] // parts).reshape((-1,) + (1,) * (len(dims) - dim - 1))

    factor_of = one(*shards[0])
    for cut in shards[1:]:
        factor_of = factor_of * one(*cut)
    return factor_of


def normal_values(rng, dims, spread, limit, pieces=(), held_as=jnp.bfloat16):
    entries = jax.random.normal(rng, dims, jnp.float32) * spread
    if len(pieces) > 0:
        entries = block_scale(rng, dims, pieces, -0.22, 0.18) * entries
    return jnp.clip(entries, min=-limit, max=limit).astype(held_as)


def setup_inputs(seed: int = 0) -> dict:
    key_of = jax.random.split(jax.random.key(seed), 11)
    resid = normal_values(key_of[0], (TOKEN_COUNT, D), 1.0, 6.0, ((0, 32),))
    queries = draw_queries(jax.random.fold_in(key_of[10], 71), 0)
    keys = draw_keys(jax.random.fold_in(key_of[10], 71), 0)
    values = normal_values(key_of[3], (TOKEN_COUNT, HEAD_COUNT * HEAD_DIM), 1.0, 6.0, ((0, 8), (1, 4)))
    cum_gate = draw_cum_gate(jax.random.fold_in(key_of[10], 71), 0)
    out_weight = normal_values(key_of[5], (HEAD_COUNT * HEAD_DIM, D), (HEAD_COUNT * HEAD_DIM // 4) ** -0.5, 0.375, ((0, 4),))
    norm_gain = jnp.clip(1.0 + 0.18 * jax.random.normal(key_of[6], (D,), jnp.float32), 0.1, 1.9)
    gate_weight = normal_values(key_of[7], (D, FF), D ** -0.5, 0.125, ((0, 8), (1, 4)))
    up_weight = normal_values(key_of[8], (D, FF), D ** -0.5, 0.125, ((0, 8), (1, 4)))
    down_weight = normal_values(key_of[9], (FF, D), FF ** -0.5, 0.078125, ((0, 4), (1, 8)))
    return dict(resid=resid, queries=queries, keys=keys, values=values, cum_gate=cum_gate, out_weight=out_weight, norm_gain=norm_gain, gate_weight=gate_weight, up_weight=up_weight, down_weight=down_weight)


def reference(resid, queries, keys, values, cum_gate, out_weight, norm_gain, gate_weight, up_weight, down_weight):
    width = HEAD_COUNT * HEAD_DIM
    total_len = queries.shape[0]
    scale = HEAD_DIM ** (-0.5)
    key_heads = keys.astype(jnp.float32).reshape(total_len, HEAD_COUNT, HEAD_DIM).transpose(1, 0, 2)
    value_heads = values.astype(jnp.float32).reshape(total_len, HEAD_COUNT, HEAD_DIM).transpose(1, 0, 2)
    key_pos = jnp.arange(total_len, dtype=jnp.int32)
    gate_rows = cum_gate.T

    def block(index):
        start = (index * TOK_DEV).astype(jnp.int32)
        query_block = lax.dynamic_slice_in_dim(queries, start, TOK_DEV, 0).astype(jnp.float32)
        query_block = query_block.reshape(TOK_DEV, HEAD_COUNT, HEAD_DIM).transpose(1, 0, 2)
        gate_block = lax.dynamic_slice_in_dim(cum_gate, start, TOK_DEV, 0).T
        score = jnp.einsum('hqd,hkd->hqk', query_block, key_heads) * scale
        score = score + gate_block[:, :, None] - gate_rows[:, None, :]
        query_pos = start + jnp.arange(TOK_DEV, dtype=jnp.int32)
        score = jnp.where(key_pos[None, None, :] <= query_pos[None, :, None], score, -jnp.inf)
        top = lax.optimization_barrier(jnp.max(score, axis=-1, keepdims=True))
        weight = jnp.exp(score - top)
        total = lax.optimization_barrier(jnp.sum(weight, axis=-1, keepdims=True))
        weight_b = lax.optimization_barrier(weight.astype(jnp.bfloat16)).astype(jnp.float32)
        numer = jnp.einsum('hqk,hkd->hqd', weight_b, value_heads)
        result = (numer / total).transpose(1, 0, 2).reshape(TOK_DEV, width)
        return result.astype(jnp.bfloat16)
    attn = lax.map(block, jnp.arange(N_SP, dtype=jnp.int32)).reshape(total_len, width)
    group = width // N_TP
    proj = jnp.zeros((total_len, D), jnp.float32)
    for index in range(N_TP):
        term = jnp.dot(attn[:, index * group:(index + 1) * group], out_weight[index * group:(index + 1) * group], preferred_element_type=jnp.float32)
        proj = proj + lax.optimization_barrier(term.astype(jnp.bfloat16)).astype(jnp.float32)
    mixed = resid.astype(jnp.float32) + proj
    normed = (mixed * lax.rsqrt(lax.optimization_barrier(jnp.mean(mixed * mixed, axis=-1, keepdims=True)) + 1e-06) * norm_gain).astype(jnp.bfloat16)
    gate = jnp.dot(normed, gate_weight, preferred_element_type=jnp.float32)
    upper = jnp.dot(normed, up_weight, preferred_element_type=jnp.float32)
    hidden = (jax.nn.silu(gate) * upper).astype(jnp.bfloat16)
    hid_group = FF // N_TP
    ffn = jnp.zeros((total_len, D), jnp.float32)
    for index in range(N_TP):
        term = jnp.dot(hidden[:, index * hid_group:(index + 1) * hid_group], down_weight[index * hid_group:(index + 1) * hid_group], preferred_element_type=jnp.float32)
        ffn = ffn + lax.optimization_barrier(term.astype(jnp.bfloat16)).astype(jnp.float32)
    return (mixed + 0.5 * ffn).astype(jnp.bfloat16)
```

```python
import functools

import jax
import jax.numpy as jnp
from jax import lax
from jax.experimental import pallas as pl
from jax.experimental.pallas import tpu as pltpu
from jax.sharding import Mesh
from jax.sharding import PartitionSpec as P

HEAD_DIM = 64
LOG2E = 1.4426950408889634


def rms_norm(mixed, norm_gain):
    scaled = mixed * lax.rsqrt(jnp.mean(mixed * mixed, axis=-1, keepdims=True) + 1e-06) * norm_gain
    return scaled.astype(jnp.bfloat16)


def rounded(term):
    return term.astype(jnp.bfloat16).astype(jnp.float32)


def flash_kernel(rows, q_block, shard_ref, q_ref, k_ref, v_ref, gate_q_ref, gate_k_ref, out_ref):
    pair = pl.program_id(0)
    block = pl.program_id(1)
    shard = shard_ref[0]
    q = q_ref[...]
    lane = lax.broadcasted_iota(jnp.int32, (q_block, 2 * HEAD_DIM), 1)
    low = lane < HEAD_DIM
    zero = jnp.zeros_like(q)
    q_heads = (jnp.where(low, q, zero), jnp.where(low, zero, q))
    gate_q = gate_q_ref[...]
    gate_lane = lax.broadcasted_iota(jnp.int32, gate_q.shape, 1)
    gates = tuple(
        jnp.sum(jnp.where(gate_lane == 2 * pair + h, gate_q, 0.0), axis=1, keepdims=True) * LOG2E
        for h in range(2)
    )
    scale = HEAD_DIM ** (-0.5) * LOG2E

    def step(j, state, masked):
        best, total, numer = state
        start = pl.multiple_of(j * rows, rows)
        k = k_ref[pl.ds(start, rows), :]
        v = v_ref[pl.ds(start, rows), :]
        new_best, new_total, parts, decay = [], [], [], []
        for h in range(2):
            s = lax.dot_general(
                q_heads[h], k, (((1,), (1,)), ((), ())), preferred_element_type=jnp.float32
            )
            gate_k = gate_k_ref[j, 0, h : h + 1, :] * LOG2E
            s = s * scale + (gates[h] - gate_k)
            if masked:
                row = lax.broadcasted_iota(jnp.int32, s.shape, 0) + block * q_block
                col = lax.broadcasted_iota(jnp.int32, s.shape, 1)
                s = jnp.where(col <= row, s, -1e30)
            top = jnp.maximum(best[h], jnp.max(s, axis=1, keepdims=True))
            keep = jnp.exp2(best[h] - top)
            w = jnp.exp2(s - top)
            new_best.append(top)
            new_total.append(total[h] * keep + jnp.sum(w, axis=1, keepdims=True))
            parts.append(
                lax.dot_general(
                    w.astype(jnp.bfloat16), v, (((1,), (0,)), ((), ())),
                    preferred_element_type=jnp.float32,
                )
            )
            decay.append(keep)
        numer = numer * jnp.where(low, decay[0], decay[1]) + jnp.where(low, parts[0], parts[1])
        return tuple(new_best), tuple(new_total), numer

    column = jnp.zeros((q_block, 1), jnp.float32)
    state = (
        (column - 1e30, column - 1e30),
        (column, column),
        jnp.zeros((q_block, 2 * HEAD_DIM), jnp.float32),
    )
    state = step(shard, state, True)
    state = lax.fori_loop(0, shard, lambda j, s: step(j, s, False), state)
    _, total, numer = state
    out_ref[...] = (numer / jnp.where(low, total[0], total[1])).astype(jnp.bfloat16)


def flash(shard, queries, kv_all, cum_gate, gates_all):
    rows, width = queries.shape
    pairs = width // (2 * HEAD_DIM)
    count = kv_all.shape[0]
    shards = count // rows
    heads = cum_gate.shape[1]
    q_block = 256 if rows % 256 == 0 else rows
    two = 2 * HEAD_DIM
    gates_all = gates_all.reshape(shards, pairs, 2, rows)
    return pl.pallas_call(
        functools.partial(flash_kernel, rows, q_block),
        grid=(pairs, rows // q_block),
        in_specs=[
            pl.BlockSpec(memory_space=pltpu.SMEM),
            pl.BlockSpec((q_block, two), lambda p, i: (i, p)),
            pl.BlockSpec((count, two), lambda p, i: (0, p)),
            pl.BlockSpec((count, two), lambda p, i: (0, pairs + p)),
            pl.BlockSpec((q_block, heads), lambda p, i: (i, 0)),
            pl.BlockSpec((shards, 1, 2, rows), lambda p, i: (0, p, 0, 0)),
        ],
        out_specs=pl.BlockSpec((q_block, two), lambda p, i: (i, p)),
        out_shape=jax.ShapeDtypeStruct((rows, width), jnp.bfloat16),
        compiler_params=pltpu.CompilerParams(vmem_limit_bytes=40 * 2**20),
        cost_estimate=pl.CostEstimate(
            flops=8 * rows * count * width,
            bytes_accessed=4 * count * width,
            transcendentals=rows * count * width // HEAD_DIM,
        ),
    )(shard.reshape(1), queries, kv_all, kv_all, cum_gate, gates_all)


def shift(value, axis, size, step):
    return lax.ppermute(value, axis, [(i, (i + step) % size) for i in range(size)])


def exchange(weight, split, joined, size):
    here = lax.axis_index("x")
    width = weight.shape[split] // size
    pieces = []
    for step in range(size):
        target = lax.rem(here + step, size)
        piece = lax.dynamic_slice_in_dim(weight, target * width, width, split)
        pieces.append(piece if step == 0 else shift(piece, "x", size, step))
    if size == 1:
        return pieces[0]
    if size == 2:
        first = here == 0
        return jnp.concatenate(
            [jnp.where(first, pieces[0], pieces[1]), jnp.where(first, pieces[1], pieces[0])], joined
        )
    length = weight.shape[joined]
    shape = list(pieces[0].shape)
    shape[joined] = length * size
    whole = jnp.zeros(shape, weight.dtype)
    for step in range(size):
        source = lax.rem(here - step + size, size)
        whole = lax.dynamic_update_slice_in_dim(whole, pieces[step], source * length, joined)
    return whole


def local(
    resid,
    queries,
    keys,
    values,
    cum_gate,
    out_weight,
    norm_gain,
    gate_weight,
    up_weight,
    down_weight,
):
    rows = queries.shape[0]
    along_x = lax.axis_size("x")
    groups = lax.axis_size("tp")
    shard = lax.axis_index("z") * along_x + lax.axis_index("x")
    gates_all = lax.all_gather(cum_gate.T, ("z", "x"), axis=0)
    kv_all = lax.all_gather(jnp.concatenate([keys, values], axis=1), ("z", "x"), axis=0, tiled=True)
    proj_weights = [out_weight] + [shift(out_weight, "tp", groups, d) for d in range(1, groups)]
    gate_cols = exchange(gate_weight, 1, 0, along_x)
    up_cols = exchange(up_weight, 1, 0, along_x)
    down_rows = exchange(down_weight, 0, 1, along_x)
    gate_full = lax.all_gather(gate_cols, "z", axis=0, tiled=True)
    up_full = lax.all_gather(up_cols, "z", axis=0, tiled=True)
    down_full = lax.all_gather(down_rows, "z", axis=1, tiled=True)

    attn = flash(shard.astype(jnp.int32), queries, kv_all, cum_gate, gates_all)

    own_rows = lax.all_to_all(attn, "tp", split_axis=0, concat_axis=1, tiled=True)
    width = attn.shape[1]
    here = lax.axis_index("tp")
    mixed = resid.astype(jnp.float32)
    for d in range(groups):
        group = lax.rem(here - d + groups, groups)
        part = lax.dynamic_slice_in_dim(own_rows, group * width, width, 1)
        mixed = mixed + rounded(
            jnp.dot(part, proj_weights[d], preferred_element_type=jnp.float32)
        )
    normed_all = lax.all_gather(rms_norm(mixed, norm_gain), ("x", "tp"), axis=0, tiled=True)
    gate_sum = jnp.dot(normed_all, gate_full, preferred_element_type=jnp.float32)
    up_sum = jnp.dot(normed_all, up_full, preferred_element_type=jnp.float32)
    hidden = (jax.nn.silu(gate_sum) * up_sum).astype(jnp.bfloat16)
    ffn_part = jnp.dot(hidden, down_full, preferred_element_type=jnp.float32)
    ffn = lax.psum_scatter(
        ffn_part.astype(jnp.bfloat16), ("x", "tp"), scatter_dimension=0, tiled=True
    ).astype(jnp.float32)
    return (mixed + 0.5 * ffn).astype(jnp.bfloat16)


def solution(mesh):
    along_sp = mesh.shape["sp"]
    along_x = 2 if along_sp % 2 == 0 else 1
    grid = Mesh(
        mesh.devices.reshape(along_sp // along_x, along_x, mesh.shape["tp"]), ("z", "x", "tp")
    )
    sp = ("z", "x")
    in_specs = (
        P(("z", "x", "tp"), None),
        P(sp, "tp"),
        P(sp, "tp"),
        P(sp, "tp"),
        P(sp, "tp"),
        P("tp", None),
        P(),
        P(sp, "tp"),
        P(sp, "tp"),
        P("tp", sp),
    )
    out_specs = P(("z", "x", "tp"), None)
    return jax.shard_map(local, mesh=grid, in_specs=in_specs, out_specs=out_specs, check_vma=False)
```

```python
import functools

import jax
import jax.numpy as jnp
from jax import lax
from jax.experimental import pallas as pl
from jax.experimental.pallas import tpu as pltpu
from jax.sharding import Mesh
from jax.sharding import PartitionSpec as P

HEAD_DIM = 64
LOG2E = 1.4426950408889634


def rms_norm(mixed, norm_gain):
    scaled = mixed * lax.rsqrt(jnp.mean(mixed * mixed, axis=-1, keepdims=True) + 1e-06) * norm_gain
    return scaled.astype(jnp.bfloat16)


def rounded(term):
    return term.astype(jnp.bfloat16).astype(jnp.float32)


def flash_kernel(rows, q_block, shard_ref, q_ref, k_ref, v_ref, gate_q_ref, gate_k_ref, out_ref):
    pair = pl.program_id(0)
    block = pl.program_id(1)
    shard = shard_ref[0]
    q = q_ref[...]
    lane = lax.broadcasted_iota(jnp.int32, (q_block, 2 * HEAD_DIM), 1)
    low = lane < HEAD_DIM
    zero = jnp.zeros_like(q)
    q_heads = (jnp.where(low, q, zero), jnp.where(low, zero, q))
    gate_q = gate_q_ref[...]
    gate_lane = lax.broadcasted_iota(jnp.int32, gate_q.shape, 1)
    gates = tuple(
        jnp.sum(jnp.where(gate_lane == 2 * pair + h, gate_q, 0.0), axis=1, keepdims=True) * LOG2E
        for h in range(2)
    )
    scale = HEAD_DIM ** (-0.5) * LOG2E

    def step(j, state, masked):
        best, total, numer = state
        start = pl.multiple_of(j * rows, rows)
        k = k_ref[pl.ds(start, rows), :]
        v = v_ref[pl.ds(start, rows), :]
        new_best, new_total, parts, decay = [], [], [], []
        for h in range(2):
            s = lax.dot_general(
                q_heads[h], k, (((1,), (1,)), ((), ())), preferred_element_type=jnp.float32
            )
            gate_k = gate_k_ref[j, 0, h : h + 1, :] * LOG2E
            s = s * scale + (gates[h] - gate_k)
            if masked:
                row = lax.broadcasted_iota(jnp.int32, s.shape, 0) + block * q_block
                col = lax.broadcasted_iota(jnp.int32, s.shape, 1)
                s = jnp.where(col <= row, s, -1e30)
            top = jnp.maximum(best[h], jnp.max(s, axis=1, keepdims=True))
            keep = jnp.exp2(best[h] - top)
            w = jnp.exp2(s - top)
            new_best.append(top)
            new_total.append(total[h] * keep + jnp.sum(w, axis=1, keepdims=True))
            parts.append(
                lax.dot_general(
                    w.astype(jnp.bfloat16), v, (((1,), (0,)), ((), ())),
                    preferred_element_type=jnp.float32,
                )
            )
            decay.append(keep)
        numer = numer * jnp.where(low, decay[0], decay[1]) + jnp.where(low, parts[0], parts[1])
        return tuple(new_best), tuple(new_total), numer

    column = jnp.zeros((q_block, 1), jnp.float32)
    state = (
        (column - 1e30, column - 1e30),
        (column, column),
        jnp.zeros((q_block, 2 * HEAD_DIM), jnp.float32),
    )
    state = step(shard, state, True)
    state = lax.fori_loop(0, shard, lambda j, s: step(j, s, False), state)
    _, total, numer = state
    out_ref[...] = (numer / jnp.where(low, total[0], total[1])).astype(jnp.bfloat16)


def flash(shard, queries, kv_all, cum_gate, gates_all):
    rows, width = queries.shape
    pairs = width // (2 * HEAD_DIM)
    count = kv_all.shape[0]
    shards = count // rows
    heads = cum_gate.shape[1]
    q_block = 256 if rows % 256 == 0 else rows
    two = 2 * HEAD_DIM
    gates_all = gates_all.reshape(shards, pairs, 2, rows)
    return pl.pallas_call(
        functools.partial(flash_kernel, rows, q_block),
        grid=(pairs, rows // q_block),
        in_specs=[
            pl.BlockSpec(memory_space=pltpu.SMEM),
            pl.BlockSpec((q_block, two), lambda p, i: (i, p)),
            pl.BlockSpec((count, two), lambda p, i: (0, p)),
            pl.BlockSpec((count, two), lambda p, i: (0, pairs + p)),
            pl.BlockSpec((q_block, heads), lambda p, i: (i, 0)),
            pl.BlockSpec((shards, 1, 2, rows), lambda p, i: (0, p, 0, 0)),
        ],
        out_specs=pl.BlockSpec((q_block, two), lambda p, i: (i, p)),
        out_shape=jax.ShapeDtypeStruct((rows, width), jnp.bfloat16),
        compiler_params=pltpu.CompilerParams(vmem_limit_bytes=40 * 2**20),
        cost_estimate=pl.CostEstimate(
            flops=8 * rows * count * width,
            bytes_accessed=4 * count * width,
            transcendentals=rows * count * width // HEAD_DIM,
        ),
    )(shard.reshape(1), queries, kv_all, kv_all, cum_gate, gates_all)


def shift(value, axis, size, step):
    return lax.ppermute(value, axis, [(i, (i + step) % size) for i in range(size)])


def exchange(weight, split, joined, size):
    here = lax.axis_index("x")
    width = weight.shape[split] // size
    pieces = []
    for step in range(size):
        target = lax.rem(here + step, size)
        piece = lax.dynamic_slice_in_dim(weight, target * width, width, split)
        pieces.append(piece if step == 0 else shift(piece, "x", size, step))
    if size == 1:
        return pieces[0]
    if size == 2:
        first = here == 0
        return jnp.concatenate(
            [jnp.where(first, pieces[0], pieces[1]), jnp.where(first, pieces[1], pieces[0])], joined
        )
    length = weight.shape[joined]
    shape = list(pieces[0].shape)
    shape[joined] = length * size
    whole = jnp.zeros(shape, weight.dtype)
    for step in range(size):
        source = lax.rem(here - step + size, size)
        whole = lax.dynamic_update_slice_in_dim(whole, pieces[step], source * length, joined)
    return whole


def local(
    resid,
    queries,
    keys,
    values,
    cum_gate,
    out_weight,
    norm_gain,
    gate_weight,
    up_weight,
    down_weight,
):
    along_x = lax.axis_size("x")
    groups = lax.axis_size("tp")
    shard = lax.axis_index("z") * along_x + lax.axis_index("x")
    gates_all = lax.all_gather(cum_gate.T, ("z", "x"), axis=0)
    kv_all = lax.all_gather(jnp.concatenate([keys, values], axis=1), ("z", "x"), axis=0, tiled=True)
    proj_weights = [out_weight] + [shift(out_weight, "tp", groups, d) for d in range(1, groups)]
    gate_cols = exchange(gate_weight, 1, 0, along_x)
    up_cols = exchange(up_weight, 1, 0, along_x)
    down_rows = exchange(down_weight, 0, 1, along_x)
    along_z = lax.axis_size("z")
    gate_full = lax.all_gather(gate_cols, "z", axis=0, tiled=True)
    up_full = lax.all_gather(up_cols, "z", axis=0, tiled=True)
    down_parts = [down_rows] + [shift(down_rows, "z", along_z, d) for d in range(1, along_z)]

    queries, gate_cols, up_cols, down_rows = lax.optimization_barrier(
        (queries, gate_cols, up_cols, down_rows)
    )
    attn = flash(shard.astype(jnp.int32), queries, kv_all, cum_gate, gates_all)

    own_rows = lax.all_to_all(attn, "tp", split_axis=0, concat_axis=1, tiled=True)
    width = attn.shape[1]
    here = lax.axis_index("tp")
    mixed = resid.astype(jnp.float32)
    for d in range(groups):
        group = lax.rem(here - d + groups, groups)
        part = lax.dynamic_slice_in_dim(own_rows, group * width, width, 1)
        mixed = mixed + rounded(
            jnp.dot(part, proj_weights[d], preferred_element_type=jnp.float32)
        )
    normed, up_full = lax.optimization_barrier((rms_norm(mixed, norm_gain), up_full))
    normed_all = lax.all_gather(normed, ("x", "tp"), axis=0, tiled=True)
    gate_sum = jnp.dot(normed_all, gate_full, preferred_element_type=jnp.float32)
    up_sum = jnp.dot(normed_all, up_full, preferred_element_type=jnp.float32)
    hidden = (jax.nn.silu(gate_sum) * up_sum).astype(jnp.bfloat16)
    ffn_part = jnp.concatenate(
        [
            jnp.dot(hidden, part, preferred_element_type=jnp.float32).astype(jnp.bfloat16)
            for part in down_parts
        ],
        axis=1,
    )
    turned = lax.psum_scatter(ffn_part, ("x", "tp"), scatter_dimension=0, tiled=True)
    block = down_parts[0].shape[1]
    ffn = jnp.concatenate(
        [
            lax.dynamic_slice_in_dim(
                turned, lax.rem(lax.axis_index("z") - c + along_z, along_z) * block, block, 1
            )
            for c in range(along_z)
        ],
        axis=1,
    ).astype(jnp.float32)
    return (mixed + 0.5 * ffn).astype(jnp.bfloat16)


def solution(mesh):
    along_sp = mesh.shape["sp"]
    along_x = 2 if along_sp % 2 == 0 else 1
    grid = Mesh(
        mesh.devices.reshape(along_sp // along_x, along_x, mesh.shape["tp"]), ("z", "x", "tp")
    )
    sp = ("z", "x")
    in_specs = (
        P(("z", "x", "tp"), None),
        P(sp, "tp"),
        P(sp, "tp"),
        P(sp, "tp"),
        P(sp, "tp"),
        P("tp", None),
        P(),
        P(sp, "tp"),
        P(sp, "tp"),
        P("tp", sp),
    )
    out_specs = P(("z", "x", "tp"), None)

    return jax.shard_map(local, mesh=grid, in_specs=in_specs, out_specs=out_specs, check_vma=False)
```
